32 devices in a mesh: sp: 4 (over y, x), tp: 8 (over z, core).
Axes of the slice: x: 2, y: 2, z: 4, core: 2. Of those that a mesh axis runs over, the one named last changes fastest.
Arguments:
- queries: bfloat16 [2048, 2048], P('sp', 'tp'), may hold values from -8 to 8
- keys: bfloat16 [2048, 1024], P('sp', 'tp'), may hold values from -8 to 8
- values: bfloat16 [2048, 1024], P('sp', 'tp'), may hold values from -6 to 6
- doc_ids: int32 [2048], P('sp'), may hold values from 0 to 1, never falling along the last dimension, each value on 1 to 1536 neighbouring positions
- sink_logits: float32 [32], P('tp'), may hold values from 3 to 6
- out_weight: bfloat16 [2048, 2048], P('tp'), may hold values from -0.75 to 0.75
- residual: bfloat16 [2048, 2048], P(('sp', 'tp')), may hold values from -6 to 6
- norm_gain: float32 [2048], replicated, may hold values from 0.1 to 1.9
- routes: int32 [2048, 2], P(('sp', 'tp')), may hold values from 0 to 3, all different within a row; in each aligned block of 64 rows (0 to 63, 64 to 127, ...) at most 36 rows name the same one
- route_weights: float32 [2048, 2], P(('sp', 'tp')), may hold values from 0.2 to 1
- gate_weight: bfloat16 [4, 2048, 7168], P('sp', None, 'tp'), may hold values from -0.125 to 0.125
- up_weight: bfloat16 [4, 2048, 7168], P('sp', None, 'tp'), may hold values from -0.125 to 0.125
- down_weight: bfloat16 [4, 7168, 2048], P('sp', 'tp'), may hold values from -0.0625 to 0.0625
Outputs:
- layer_output: bfloat16 [2048, 2048], P(('sp', 'tp'))
The draws below stay inside these ranges and needn't reach their ends.
Inputs may be any that keep to these rules, and one draw needn't show every extreme that they name: `doc_ids`: never falling along the sequence; each document spans 1 to 1536 positions, one exactly that many. `routes`: each row names 2 different experts. In the rows of one device (aligned blocks of 64 rows) no expert is named by more than 36 rows, a bound that some block reaches.
All inputs are finite; a program needn't handle non-finite values.
Results may differ from the reference program's by a relative error of at most 0.015.
Values may be sent and summed in bfloat16 or wider, within the bound.
A program may use at most 128 MiB of HBM per device.

```python
import math
import jax
import jax.numpy as jnp
import numpy as np
from jax import lax

D = 2048
HEADS = 32
KV_HEADS = 16
HEAD_DIM = 64
WINDOW = 128
FF = 7168
TOP_K = 2
TOK_DEV = 64
TOK_SP = 512
SEQ = 2048
EXPERTS = 4
CAP = 36
DOCS = 2
N_TP = 8


def draw_queries(key, part):
    normal_values = jnp.clip(jax.random.normal(jax.random.fold_in(key, 1), (SEQ, HEADS * HEAD_DIM), jnp.float32), -6.0, 6.0)
    return normal_values.astype(jnp.bfloat16)


def draw_keys(key, part):
    normal_values = jnp.clip(jax.random.normal(jax.random.fold_in(key, 2), (SEQ, KV_HEADS * HEAD_DIM), jnp.float32), -6.0, 6.0)
    return normal_values.astype(jnp.bfloat16)


def block_scale(rng, dims, cuts, smallest, top_value):
    level = 1.0
    for axis_at, parts in cuts:
        heights = jax.random.uniform(jax.random.fold_in(jax.random.fold_in(rng, 6), axis_at), (parts,), jnp.float32, smallest / len(cuts), top_value / len(cuts))
        level = level * jnp.repeat(jnp.exp(heights), dims[axis_at] // parts).reshape((-1,) + (1,) * (len(dims) - 1 - axis_at))
    return level


def length_profile(amount, total, limit, skew):
    portions = [(1 << 20) // math.isqrt(grade ** skew) + 1 for grade in range(2, amount + 1)]
    surplus, given = total - limit - (amount - 1), [1] * (amount - 1)
    while surplus > 0:
        movable = [i for i in range(amount - 1) if given[i] < limit]
        mass, remaining = sum([portions[i] for i in movable]), surplus
        for i in movable:
            more = min(limit - given[i], max(1, remaining * portions[i] // mass), surplus)
            given[i] = given[i] + more
            surplus = surplus - more
    return np.array([limit] + given)


def ragged_sizes(stream_key, number_of, total, most, skew):
    if number_of == 2:
        one = jax.random.randint(stream_key, (), max(1, total - most), min(most, total - 1) + 1)
        return jnp.stack([one, total - one])
    lengths = jnp.asarray(length_profile(number_of, total, most, skew), jnp.int32)
    twos = (number_of - 1) // 2
    donor, sink = lengths[1:1 + 2 * twos:2], lengths[2:2 + 2 * twos:2]
    slack = jnp.minimum(donor - 1, most - sink)
    passed = jax.random.randint(jax.random.fold_in(stream_key, 1), (twos,), 0, 1 << 20) % (slack + 1)
    lengths = lengths.at[1:1 + 2 * twos:2].set(donor - passed).at[2:2 + 2 * twos:2].set(sink + passed)
    return lengths[jax.random.permutation(jax.random.fold_in(stream_key, 2), number_of)]


def deal_out(own_key, own, number, rows, number_of, top, reach, lean):
    order = jax.random.permutation(own_key, number_of)
    heavy_load, ordinary = load_shares(number_of, rows * top, reach, lean, True), load_shares(number_of, rows * top, reach, lean, False)
    places = jnp.arange(number_of)

    def named(sizes, turn):
        used = int((sizes > 0).sum())
        fixed = max(1, used // 4)
        passed = fixed + (places - fixed + turn * (used - fixed)) % max(1, number_of - fixed)
        return jnp.zeros((number_of,), jnp.int32).at[order[jnp.where(places < fixed, places, passed)]].set(jnp.asarray(sizes, jnp.int32))

    sizes = jnp.where(number % 4 == 0, named(heavy_load, number // 4), named(ordinary, number - number // 4 - 1))
    mixed = jax.random.permutation(jax.random.fold_in(own, 3), number_of)
    donor, sink = mixed[0:number_of // 2 * 2:2], mixed[1:number_of // 2 * 2:2]
    margin = jnp.minimum(sizes[donor] - 1, reach - sizes[sink]) // 2
    margin = jnp.where((donor == order[0]) | (sink == order[0]) | (sizes[sink] == 0), 0, jnp.maximum(margin, 0))
    passed = jax.random.randint(jax.random.fold_in(own, 4), (number_of // 2,), 0, 1 << 20) % (margin + 1)
    sizes = sizes.at[donor].add(-passed).at[sink].add(passed)
    labels = jnp.searchsorted(jnp.cumsum(sizes), jnp.arange(rows * top), side="right").astype(jnp.int32)
    listing = labels.reshape(top, rows).T
    listing = listing[jax.random.permutation(jax.random.fold_in(own, 1), rows)]
    turn = jax.random.randint(jax.random.fold_in(own, 2), (rows, 1), 0, top)
    return jnp.take_along_axis(listing, (jnp.arange(top)[None, :] + turn) % top, axis=1)


def load_shares(number_of, total, limit, skew, full):
    loads = [(1 << 20) // math.isqrt(rank ** skew) + 1 for rank in range(1, number_of + 1)]
    largest = limit if full else min(limit, max(-(-total // number_of), total * loads[0] // sum(loads)))
    least = 1 if total - largest >= number_of - 1 else 0
    counts, surplus = [largest] + [least] * (number_of - 1), total - largest - least * (number_of - 1)
    while surplus > 0:
        free = [i for i in range(1, number_of) if counts[i] < largest] or [i for i in range(1, number_of) if counts[i] < limit]
        mass, left = sum([loads[i] for i in free]), surplus
        for i in free:
            extra = min(limit - counts[i], max(1, left * loads[i] // mass), surplus)
            counts[i] = counts[i] + extra
            surplus = surplus - extra
    return np.array(counts)


def noise(own_key, extent, scale, reach, cuts=(), kind=jnp.bfloat16):
    entries = scale * jax.random.normal(own_key, extent, jnp.float32)
    if cuts:
        entries = entries * block_scale(own_key, extent, cuts, -0.22, 0.18)
    return jnp.clip(entries, -reach, reach).astype(kind)


def setup_inputs(seed: int = 0) -> dict:
    key_of = jax.random.split(jax.random.key(seed), 14)
    queries = draw_queries(jax.random.fold_in(key_of[13], 71), 0)
    keys = draw_keys(jax.random.fold_in(key_of[13], 71), 0)
    values = noise(key_of[2], (SEQ, KV_HEADS * HEAD_DIM), 1.0, 6.0, ((0, 4), (1, 8)))
    doc_ids = jnp.searchsorted(jnp.cumsum(ragged_sizes(key_of[3], DOCS, SEQ, 3 * TOK_SP, 1)), jnp.arange(SEQ), side="right").astype(jnp.int32)
    sink_logits = jnp.clip(3.0 + 3.0 * jax.random.uniform(key_of[4], (HEADS,), jnp.float32) ** block_scale(key_of[4], (HEADS,), ((0, 8),), -0.2, 0.2), 3.0, 6.0)
    out_weight = noise(key_of[5], (HEADS * HEAD_DIM, D), HEAD_DIM ** -0.5, 0.75, ((0, 8),))
    residual = noise(key_of[6], (SEQ, D), 1.0, 6.0, ((0, 32),))
    norm_gain = jnp.clip(1.0 + 0.18 * jax.random.normal(key_of[7], (D,), jnp.float32), 0.1, 1.9)
    routes_keys = jax.random.split(jax.random.fold_in(key_of[8], 1), SEQ // TOK_DEV)
    routes_turns = jax.random.permutation(jax.random.fold_in(key_of[8], 3), SEQ // TOK_DEV)
    routes = jax.vmap(lambda own, number: deal_out(jax.random.fold_in(key_of[8], 2), own, number, TOK_DEV, EXPERTS, TOP_K, CAP, 2))(routes_keys, routes_turns).reshape((SEQ, TOP_K))
    route_weights = jnp.clip(0.2 + 0.8 * jax.random.uniform(key_of[9], (SEQ, TOP_K), jnp.float32) ** block_scale(key_of[9], (SEQ, TOP_K), ((0, 32),), -0.2, 0.2), 0.2, 1.0)
    gate_weight = noise(key_of[10], (EXPERTS, D, FF), D ** -0.5, 0.125, ((0, 4), (2, 8)))
    up_weight = noise(key_of[11], (EXPERTS, D, FF), D ** -0.5, 0.125, ((0, 4), (2, 8)))
    down_weight = noise(key_of[12], (EXPERTS, FF, D), FF ** -0.5, 0.0625, ((0, 4), (1, 8)))
    return dict(queries=queries, keys=keys, values=values, doc_ids=doc_ids, sink_logits=sink_logits, out_weight=out_weight, residual=residual, norm_gain=norm_gain, routes=routes, route_weights=route_weights, gate_weight=gate_weight, up_weight=up_weight, down_weight=down_weight)


layer_epsilon = 1e-05
masked_score = -1e+30

def reference(queries, keys, values, doc_ids, sink_logits, out_weight, residual, norm_gain, routes, route_weights, gate_weight, up_weight, down_weight):
    reach_back = WINDOW - 1
    group_ratio = HEADS // KV_HEADS
    block_rows = min(512, TOK_SP)
    score_scale = 1.0 / math.sqrt(HEAD_DIM)
    kv_width = KV_HEADS * HEAD_DIM
    padded_keys = jnp.concatenate([jnp.zeros((reach_back, kv_width), keys.dtype), keys], axis=0)
    padded_values = jnp.concatenate([jnp.zeros((reach_back, kv_width), values.dtype), values], axis=0)
    padded_docs = jnp.concatenate([jnp.full((reach_back,), -1, jnp.int32), doc_ids.astype(jnp.int32)], axis=0)
    sink_table = sink_logits.astype(jnp.float32).reshape(KV_HEADS, group_ratio, 1)

    def attend_block(block_index):
        first_row = (block_index * block_rows).astype(jnp.int32)
        query_rows = lax.dynamic_slice_in_dim(queries, first_row, block_rows, 0).astype(jnp.float32)
        query_rows = query_rows.reshape(block_rows, KV_HEADS, group_ratio, HEAD_DIM)
        key_rows = lax.dynamic_slice_in_dim(padded_keys, first_row, block_rows + reach_back, 0).astype(jnp.float32)
        key_rows = key_rows.reshape(block_rows + reach_back, KV_HEADS, HEAD_DIM)
        value_rows = lax.dynamic_slice_in_dim(padded_values, first_row, block_rows + reach_back, 0).astype(jnp.float32)
        value_rows = value_rows.reshape(block_rows + reach_back, KV_HEADS, HEAD_DIM)
        query_docs = lax.dynamic_slice_in_dim(doc_ids.astype(jnp.int32), first_row, block_rows, 0)
        key_docs = lax.dynamic_slice_in_dim(padded_docs, first_row, block_rows + reach_back, 0)
        scores = jnp.einsum('bgrd,sgd->grbs', query_rows, key_rows) * score_scale
        offsets = jnp.arange(block_rows)[:, None] + reach_back - jnp.arange(block_rows + reach_back)[None, :]
        allowed = (offsets >= 0) & (offsets <= reach_back) & (query_docs[:, None] == key_docs[None, :])
        scores = jnp.where(allowed, scores, masked_score)
        row_max = jnp.maximum(scores.max(-1), sink_table)
        exp_scores = jnp.exp(scores - row_max[..., None])
        denominator = exp_scores.sum(-1) + jnp.exp(sink_table - row_max)
        probabilities = lax.optimization_barrier(exp_scores.astype(jnp.bfloat16)).astype(jnp.float32)
        weighted = jnp.einsum('grbs,sgd->bgrd', probabilities, value_rows)
        weighted = weighted / jnp.transpose(denominator, (2, 0, 1))[..., None]
        return weighted.astype(jnp.bfloat16).reshape(block_rows, HEADS * HEAD_DIM)
    attended = lax.map(attend_block, jnp.arange(SEQ // block_rows, dtype=jnp.int32)).reshape(SEQ, HEADS * HEAD_DIM)
    projected = jnp.dot(attended, out_weight, preferred_element_type=jnp.float32)
    stream = residual.astype(jnp.float32) + projected
    mean_value = stream.mean(-1, keepdims=True)
    centred = stream - mean_value
    variance = (centred * centred).mean(-1, keepdims=True)
    normed = (centred * lax.rsqrt(variance + layer_epsilon) * norm_gain.astype(jnp.float32)).astype(jnp.bfloat16)
    blocks_total = SEQ // TOK_DEV
    flat_routes = routes.astype(jnp.int32).reshape(blocks_total, TOP_K * TOK_DEV)
    one_hot = (flat_routes[..., None] == jnp.arange(EXPERTS, dtype=jnp.int32)).astype(jnp.int32)
    slot_ids = lax.optimization_barrier(jnp.sum((jnp.cumsum(one_hot, axis=1) - 1) * one_hot, axis=-1))
    block_base = jnp.arange(blocks_total, dtype=jnp.int32)[:, None] * CAP
    destination = (flat_routes * (blocks_total * CAP) + block_base + slot_ids).reshape(-1).astype(jnp.int32)
    token_index = (jnp.arange(SEQ * TOP_K, dtype=jnp.int32) // TOP_K).astype(jnp.int32)
    buffer_rows = jnp.zeros((EXPERTS * blocks_total * CAP, D), jnp.bfloat16).at[destination].set(normed[token_index])

    def run_expert(expert_index):
        rows_in = lax.dynamic_slice_in_dim(buffer_rows, (expert_index * blocks_total * CAP).astype(jnp.int32), blocks_total * CAP, 0)
        gate = jnp.dot(rows_in, gate_weight[expert_index], preferred_element_type=jnp.float32)
        upward = jnp.dot(rows_in, up_weight[expert_index], preferred_element_type=jnp.float32)
        hidden = (jax.nn.silu(gate) * upward).astype(jnp.bfloat16)
        grouped = hidden.reshape(blocks_total * CAP, N_TP, FF // N_TP).astype(jnp.float32)
        down_groups = down_weight[expert_index].reshape(N_TP, FF // N_TP, D).astype(jnp.float32)
        partials = jnp.einsum('rtf,tfd->trd', grouped, down_groups)
        rounded = lax.optimization_barrier(partials.astype(jnp.bfloat16)).astype(jnp.float32)
        return rounded.sum(0).astype(jnp.bfloat16)
    results = lax.map(run_expert, jnp.arange(EXPERTS, dtype=jnp.int32)).reshape(EXPERTS * blocks_total * CAP, D)
    picked = results[destination].astype(jnp.float32).reshape(SEQ, TOP_K, D)
    combined = lax.optimization_barrier(jnp.sum(picked * route_weights.astype(jnp.float32)[..., None], axis=1))
    return (stream + combined).astype(jnp.bfloat16)
```

```python
import functools
import math

import jax
import jax.numpy as jnp
from jax import lax
from jax.experimental import pallas as pl
from jax.experimental.pallas import tpu as pltpu
from jax.sharding import PartitionSpec as P

HEAD_DIM = 64
WINDOW = 128


layer_epsilon = 1e-05
masked_score = -1e30


def passed_along(value, axis, steps):
    count = lax.axis_size(axis)
    first, last = (max(0, -steps), min(count, count - steps))
    return lax.ppermute(value, axis, [(source, source + steps) for source in range(first, last)])


VMEM = pl.BlockSpec(memory_space=pltpu.VMEM)


def remote(source, target, sent, landed, device):
    return pltpu.make_async_remote_copy(
        src_ref=source,
        dst_ref=target,
        send_sem=sent,
        recv_sem=landed,
        device_id=device,
        device_id_type=pl.DeviceIdType.MESH,
    )


def tp_place():
    me = lax.axis_index("tp")
    chip, core = me // 2, lax.rem(me, 2)
    return chip, core, chip * 2 + 1 - core, me - 2, me + 2


def greet(chips, spans):
    chip, _, partner, before, after = tp_place()
    span = lax.axis_index("sp")
    barrier = pltpu.get_barrier_semaphore()

    def hello(device):
        pl.semaphore_signal(
            barrier, inc=1, device_id=device, device_id_type=pl.DeviceIdType.MESH
        )

    hello({"tp": partner})
    pl.when(chip > 0)(lambda: hello({"tp": before}))
    pl.when(chip < chips - 1)(lambda: hello({"tp": after}))
    for step in range(1, spans):
        hello({"sp": lax.rem(span + step, spans)})
    inner = jnp.where(chip > 0, 1, 0) + jnp.where(chip < chips - 1, 1, 0)
    pl.semaphore_wait(barrier, inner + spans)


def outside_in(count):
    order = []
    for step in range((count + 1) // 2):
        order.extend([count - 1 - step] + ([step] if step != count - 1 - step else []))
    return order


def column_loop(width, body):
    step = min(512, width)

    def one(index, carry):
        body(pl.ds(pl.multiple_of(index * step, step), step))
        return carry

    lax.fori_loop(0, width // step, one, 0)


def line_step(chips, block, term, width, total, travel, held, sent, landed):
    chip, _, _, before, after = tp_place()
    for way, passes, receives, device in (
        (0, chip < block, chip > 0, {"tp": after}),
        (1, chip > block, chip < chips - 1, {"tp": before}),
    ):
        copy = remote(
            travel.at[block], held.at[way, block], sent.at[block], landed.at[way, block], device
        )

        @pl.when(passes & receives)
        def _(copy=copy, way=way):
            copy.wait_recv()

            def add(columns):
                travel[block, :, columns] = (
                    term(columns) + held[way, block, :, columns].astype(jnp.float32)
                ).astype(jnp.bfloat16)

            column_loop(width, add)

        @pl.when(passes & jnp.logical_not(receives))
        def _():
            def keep(columns):
                travel[block, :, columns] = term(columns).astype(jnp.bfloat16)

            column_loop(width, keep)

        pl.when(passes)(copy.start)

    @pl.when(chip == block)
    def _():
        def keep(columns):
            total[:, columns] = term(columns)

        column_loop(width, keep)


def line_finish(chips, width, total, travel, held, sent, landed):
    chip, _, _, before, after = tp_place()
    for way, receives in ((0, chip > 0), (1, chip < chips - 1)):

        @pl.when(receives)
        def _(way=way):
            remote(
                travel.at[chip],
                held.at[way, chip],
                sent.at[chip],
                landed.at[way, chip],
                {"tp": after},
            ).wait_recv()

            def add(columns):
                total[:, columns] = total[:, columns] + held[way, chip, :, columns].astype(
                    jnp.float32
                )

            column_loop(width, add)

    for block in range(chips):
        copy = remote(
            travel.at[block], held.at[0, block], sent.at[block], landed.at[0, block], {"tp": after}
        )
        pl.when(chip != block)(copy.wait_send)


def sum_kernel(
    chips, parts, total, arrived, travel, held, core_sent, core_landed, sent, landed
):
    _, core, partner, _, _ = tp_place()
    width = parts.shape[-1]
    greet(chips, 1)

    def handed(block):
        return remote(
            parts.at[block, 1 - core],
            arrived.at[block],
            core_sent.at[block],
            core_landed.at[block],
            {"tp": partner},
        )

    for block in outside_in(chips):
        handed(block).start()
    for block in outside_in(chips):
        handed(block).wait_recv()

        def term(columns, block=block):
            return parts[block, core, :, columns].astype(jnp.float32) + arrived[
                block, :, columns
            ].astype(jnp.float32)

        line_step(chips, block, term, width, total, travel, held, sent, landed)
    line_finish(chips, width, total, travel, held, sent, landed)
    for block in range(chips):
        handed(block).wait_send()


def tp_sum(parts):
    chips, _, rows, width = parts.shape
    dma = pltpu.SemaphoreType.DMA
    return pl.pallas_call(
        functools.partial(sum_kernel, chips),
        out_shape=jax.ShapeDtypeStruct((rows, width), jnp.float32),
        in_specs=[VMEM],
        out_specs=VMEM,
        scratch_shapes=[
            pltpu.VMEM((chips, rows, width), jnp.bfloat16),
            pltpu.VMEM((chips, rows, width), jnp.bfloat16),
            pltpu.VMEM((2, chips, rows, width), jnp.bfloat16),
            dma((chips,)),
            dma((chips,)),
            dma((chips,)),
            dma((2, chips)),
        ],
        compiler_params=pltpu.CompilerParams(
            collective_id=0, has_side_effects=True, vmem_limit_bytes=60 << 20
        ),
    )(parts)


def spread_kernel(
    chips,
    spans,
    picks,
    normed,
    notes,
    rows,
    all_notes,
    blocks,
    outgoing,
    line_sent,
    line_landed,
    note_sent,
    note_landed,
    span_sent,
    span_landed,
    core_sent,
    core_landed,
):
    chip, core, partner, before, after = tp_place()
    span = lax.axis_index("sp")
    count, width = normed.shape
    slots = rows.shape[3]
    greet(chips, spans)
    all_notes[chip] = notes[...]

    def pass_on(block, way, first):
        device = {"tp": after if way == 0 else before}
        return (
            remote(
                normed if first else blocks.at[block],
                blocks.at[block],
                line_sent.at[way, block],
                line_landed.at[block],
                device,
            ),
            remote(
                notes if first else all_notes.at[block],
                all_notes.at[block],
                note_sent.at[way, block],
                note_landed.at[block],
                device,
            ),
        )

    def to_span(block, step):
        other = lax.rem(span + step, spans)
        return remote(
            outgoing.at[block, other],
            rows.at[core, block, span],
            span_sent.at[block, step],
            span_landed.at[block, step],
            {"sp": other},
        )

    def to_partner(block):
        return remote(
            rows.at[core, block],
            rows.at[core, block],
            core_sent.at[block],
            core_landed.at[block],
            {"tp": partner},
        )

    def hand_out(block, source, note):
        listing = note[...][:picks, :count]
        for expert in range(spans):
            slot = (
                lax.broadcasted_iota(jnp.int32, (slots, count), 0) + expert * slots
            ).astype(jnp.float32)
            chosen = jnp.zeros((slots, count), jnp.float32)
            for pick in range(picks):
                chosen = jnp.where(slot == listing[pick : pick + 1], 1.0, chosen)
            chosen = chosen.astype(jnp.bfloat16)

            def select(columns, expert=expert, chosen=chosen):
                outgoing[block, expert, :, columns] = jnp.dot(
                    chosen, source[:, columns], preferred_element_type=jnp.float32
                ).astype(jnp.bfloat16)

            column_loop(width, select)
        for step in range(1, spans):
            to_span(block, step).start()
        rows[core, block, span] = outgoing[block, span]

    def start_both(block, way, first):
        for copy in pass_on(block, way, first):
            copy.start()

    pl.when(chip < chips - 1)(lambda: start_both(chip, 0, True))
    pl.when(chip > 0)(lambda: start_both(chip, 1, True))
    hand_out(chip, normed, notes)
    for step in range(1, chips):
        for way, block, present, further in (
            (0, chip - step, chip >= step, chip < chips - 1),
            (1, chip + step, chip + step < chips, chip > 0),
        ):

            @pl.when(present)
            def _(way=way, block=block, further=further):
                for copy in pass_on(block, way, False):
                    copy.wait_recv()
                pl.when(further)(lambda: start_both(block, way, False))
                hand_out(block, blocks.at[block], all_notes.at[block])

    def finish(block):
        for step in range(1, spans):
            to_span(block, step).wait_recv()
        to_partner(block).start()

    finish(chip)
    for step in range(1, chips):
        pl.when(chip >= step)(lambda step=step: finish(chip - step))
        pl.when(chip + step < chips)(lambda step=step: finish(chip + step))

    def wait_both(block, way, first):
        for copy in pass_on(block, way, first):
            copy.wait_send()

    for block in range(chips):
        pl.when((chip >= block) & (chip < chips - 1))(lambda block=block: wait_both(block, 0, False))
        pl.when((chip <= block) & (chip > 0))(lambda block=block: wait_both(block, 1, False))
        for step in range(1, spans):
            to_span(block, step).wait_send()
        to_partner(block).wait()


def spread(normed, notes, chips, spans, slots, picks):
    count, width = normed.shape
    dma = pltpu.SemaphoreType.DMA
    return pl.pallas_call(
        functools.partial(spread_kernel, chips, spans, picks),
        out_shape=(
            jax.ShapeDtypeStruct((2, chips, spans, slots, width), jnp.bfloat16),
            jax.ShapeDtypeStruct((chips,) + notes.shape, jnp.float32),
        ),
        in_specs=[VMEM, VMEM],
        out_specs=(VMEM, VMEM),
        scratch_shapes=[
            pltpu.VMEM((chips, count, width), jnp.bfloat16),
            pltpu.VMEM((chips, spans, slots, width), jnp.bfloat16),
            dma((2, chips)),
            dma((chips,)),
            dma((2, chips)),
            dma((chips,)),
            dma((chips, spans)),
            dma((chips, spans)),
            dma((chips,)),
            dma((chips,)),
        ],
        compiler_params=pltpu.CompilerParams(
            collective_id=1, has_side_effects=True, vmem_limit_bytes=60 << 20
        ),
    )(normed, notes)


def collect_kernel(
    chips,
    spans,
    parts,
    shares,
    total,
    arrived,
    outgoing,
    gathered,
    travel,
    held,
    core_sent,
    core_landed,
    span_sent,
    span_landed,
    sent,
    landed,
):
    _, core, partner, _, _ = tp_place()
    span = lax.axis_index("sp")
    width = parts.shape[-1]
    greet(chips, spans)

    def handed(block):
        return remote(
            parts.at[1 - core, block],
            arrived.at[block],
            core_sent.at[block],
            core_landed.at[block],
            {"tp": partner},
        )

    def to_span(block, step):
        other = lax.rem(span + step, spans)
        return remote(
            outgoing.at[block, other],
            gathered.at[block, span],
            span_sent.at[block, step],
            span_landed.at[block, step],
            {"sp": other},
        )

    for block in outside_in(chips):
        handed(block).start()
    for block in outside_in(chips):
        handed(block).wait_recv()

        def add(columns, block=block):
            outgoing[block, :, :, columns] = (
                parts[core, block, :, :, columns].astype(jnp.float32)
                + arrived[block, :, :, columns].astype(jnp.float32)
            ).astype(jnp.bfloat16)

        column_loop(width, add)
        for step in range(1, spans):
            to_span(block, step).start()
        gathered[block, span] = outgoing[block, span]
    for block in outside_in(chips):
        for step in range(1, spans):
            to_span(block, step).wait_recv()

        def term(columns, block=block):
            result = None
            for expert in range(spans):
                share = jnp.dot(
                    shares[block, expert],
                    gathered[block, expert, :, columns],
                    preferred_element_type=jnp.float32,
                )
                result = share if result is None else result + share
            return result

        line_step(chips, block, term, width, total, travel, held, sent, landed)
    line_finish(chips, width, total, travel, held, sent, landed)
    for block in range(chips):
        handed(block).wait_send()
        for step in range(1, spans):
            to_span(block, step).wait_send()


def collect(parts, shares):
    _, chips, spans, slots, width = parts.shape
    rows = shares.shape[2]
    dma = pltpu.SemaphoreType.DMA
    return pl.pallas_call(
        functools.partial(collect_kernel, chips, spans),
        out_shape=jax.ShapeDtypeStruct((rows, width), jnp.float32),
        in_specs=[VMEM, VMEM],
        out_specs=VMEM,
        scratch_shapes=[
            pltpu.VMEM((chips, spans, slots, width), jnp.bfloat16),
            pltpu.VMEM((chips, spans, slots, width), jnp.bfloat16),
            pltpu.VMEM((chips, spans, slots, width), jnp.bfloat16),
            pltpu.VMEM((chips, rows, width), jnp.bfloat16),
            pltpu.VMEM((2, chips, rows, width), jnp.bfloat16),
            dma((chips,)),
            dma((chips,)),
            dma((chips, spans)),
            dma((chips, spans)),
            dma((chips,)),
            dma((2, chips)),
        ],
        compiler_params=pltpu.CompilerParams(
            collective_id=2, has_side_effects=True, vmem_limit_bytes=60 << 20
        ),
    )(parts, shares)


def local(
    queries,
    keys,
    values,
    doc_ids,
    sink_logits,
    out_weight,
    residual,
    norm_gain,
    routes,
    route_weights,
    gate_weight,
    up_weight,
    down_weight,
):
    span_rows = queries.shape[0]
    kv_width = keys.shape[1]
    kv_groups = kv_width // HEAD_DIM
    heads_here = queries.shape[1] // HEAD_DIM
    group_ratio = heads_here // kv_groups
    reach_back = WINDOW - 1
    score_scale = 1.0 / math.sqrt(HEAD_DIM)
    doc_float = (doc_ids + 1).astype(jnp.float32)
    key_value = jnp.concatenate([keys, values], axis=1).astype(jnp.float32)
    tail_pairs, tail_docs = (
        passed_along(key_value[span_rows - reach_back :].astype(jnp.bfloat16), "sp", 1).astype(
            jnp.float32
        ),
        passed_along(doc_float[span_rows - reach_back :].astype(jnp.bfloat16), "sp", 1).astype(
            jnp.float32
        ),
    )
    all_keys = jnp.concatenate([tail_pairs[:, :kv_width].astype(jnp.bfloat16), keys], axis=0)
    all_values = jnp.concatenate([tail_pairs[:, kv_width:].astype(jnp.bfloat16), values], axis=0)
    all_docs = jnp.concatenate([tail_docs, doc_float], axis=0)
    block_rows = min(512, span_rows)
    sink_table = sink_logits.reshape(kv_groups, group_ratio, 1)
    offsets = (
        jnp.arange(block_rows)[:, None] + reach_back - jnp.arange(block_rows + reach_back)[None, :]
    )
    window_mask = (offsets >= 0) & (offsets <= reach_back)
    pieces = []
    for block_index in range(span_rows // block_rows):
        first_row = block_index * block_rows
        query_rows = queries[first_row : first_row + block_rows].reshape(
            block_rows, kv_groups, group_ratio, HEAD_DIM
        )
        key_rows = all_keys[first_row : first_row + block_rows + reach_back].reshape(
            block_rows + reach_back, kv_groups, HEAD_DIM
        )
        value_rows = all_values[first_row : first_row + block_rows + reach_back].reshape(
            block_rows + reach_back, kv_groups, HEAD_DIM
        )
        scores = (
            jnp.einsum("bgrd,sgd->grbs", query_rows, key_rows, preferred_element_type=jnp.float32)
            * score_scale
        )
        same_doc = (
            doc_float[first_row : first_row + block_rows][:, None]
            == all_docs[first_row : first_row + block_rows + reach_back][None, :]
        )
        scores = jnp.where(window_mask & same_doc, scores, masked_score)
        row_max = jnp.maximum(scores.max(-1), sink_table)
        exp_scores = jnp.exp(scores - row_max[..., None])
        denominator = exp_scores.sum(-1) + jnp.exp(sink_table - row_max)
        weighted = jnp.einsum(
            "grbs,sgd->bgrd",
            exp_scores.astype(jnp.bfloat16),
            value_rows,
            preferred_element_type=jnp.float32,
        )
        weighted = weighted / jnp.transpose(denominator, (2, 0, 1))[..., None]
        pieces.append(weighted.astype(jnp.bfloat16).reshape(block_rows, heads_here * HEAD_DIM))
    attended = jnp.concatenate(pieces, axis=0)
    rows_here = attended
    token_count, width = residual.shape
    chips = lax.axis_size("tp") // 2
    projected = tp_sum(
        jnp.dot(rows_here, out_weight, preferred_element_type=jnp.float32)
        .astype(jnp.bfloat16)
        .reshape(chips, 2, token_count, width)
    )
    stream = residual.astype(jnp.float32) + projected
    mean_value = stream.mean(-1, keepdims=True)
    centred = stream - mean_value
    variance = (centred * centred).mean(-1, keepdims=True)
    normed = (centred * lax.rsqrt(variance + layer_epsilon) * norm_gain).astype(jnp.bfloat16)
    spans = lax.axis_size("sp")
    route_count = routes.shape[1]
    capacity = 9 * route_count * token_count // (8 * spans)
    slots = -(-capacity // 8) * 8
    flat_routes = routes.reshape(-1)
    one_hot = (flat_routes[:, None] == jnp.arange(spans)[None, :]).astype(jnp.int32)
    slot_ids = jnp.sum((jnp.cumsum(one_hot, axis=0) - 1) * one_hot, axis=1)
    destination = (flat_routes * slots + slot_ids).astype(jnp.float32)
    notes = jnp.concatenate(
        [destination.reshape(token_count, route_count).T, route_weights.T], axis=0
    )
    notes = jnp.pad(
        notes,
        ((0, -2 * route_count % 8), (0, -token_count % 128)),
        constant_values=-1.0,
    )
    arrived, all_notes = spread(normed, notes, chips, spans, slots, route_count)
    rows_in = arrived.reshape(-1, width)
    gate = jnp.dot(rows_in, gate_weight[0], preferred_element_type=jnp.float32)
    upward = jnp.dot(rows_in, up_weight[0], preferred_element_type=jnp.float32)
    hidden = (jax.nn.silu(gate) * upward).astype(jnp.bfloat16)
    partial_value = jnp.dot(hidden, down_weight[0], preferred_element_type=jnp.float32).astype(
        jnp.bfloat16
    )
    places = all_notes[:, None, :route_count, :token_count, None]
    weights = all_notes[:, None, route_count : 2 * route_count, :token_count, None]
    slot_range = jnp.arange(spans * slots).astype(jnp.float32).reshape(1, spans, 1, 1, slots)
    shares = jnp.sum(jnp.where(places == slot_range, weights, 0.0), axis=2).astype(jnp.bfloat16)
    combined = collect(partial_value.reshape(arrived.shape), shares)
    return (stream + combined).astype(jnp.bfloat16)


def solution(mesh):
    placed = (
        P("sp", "tp"),
        P("sp", "tp"),
        P("sp", "tp"),
        P("sp"),
        P("tp"),
        P("tp", None),
        P(("sp", "tp"), None),
        P(),
        P(("sp", "tp"), None),
        P(("sp", "tp"), None),
        P("sp", None, "tp"),
        P("sp", None, "tp"),
        P("sp", "tp", None),
    )
    return jax.shard_map(
        local, mesh=mesh, in_specs=placed, out_specs=P(("sp", "tp"), None), check_vma=False
    )
```

```python
import functools
import math

import jax
import jax.numpy as jnp
from jax import lax
from jax.experimental import pallas as pl
from jax.experimental.pallas import tpu as pltpu
from jax.sharding import PartitionSpec as P

HEAD_DIM = 64
WINDOW = 128


layer_epsilon = 1e-05
masked_score = -1e30


def passed_along(value, axis, steps):
    count = lax.axis_size(axis)
    first, last = (max(0, -steps), min(count, count - steps))
    return lax.ppermute(value, axis, [(source, source + steps) for source in range(first, last)])


VMEM = pl.BlockSpec(memory_space=pltpu.VMEM)


def remote(source, target, sent, landed, device):
    return pltpu.make_async_remote_copy(
        src_ref=source,
        dst_ref=target,
        send_sem=sent,
        recv_sem=landed,
        device_id=device,
        device_id_type=pl.DeviceIdType.MESH,
    )


def tp_place():
    me = lax.axis_index("tp")
    chip, core = me // 2, lax.rem(me, 2)
    return chip, core, chip * 2 + 1 - core, me - 2, me + 2


def greet(chips, spans):
    chip, _, partner, before, after = tp_place()
    span = lax.axis_index("sp")
    barrier = pltpu.get_barrier_semaphore()

    def hello(device):
        pl.semaphore_signal(
            barrier, inc=1, device_id=device, device_id_type=pl.DeviceIdType.MESH
        )

    hello({"tp": partner})
    pl.when(chip > 0)(lambda: hello({"tp": before}))
    pl.when(chip < chips - 1)(lambda: hello({"tp": after}))
    for step in range(1, spans):
        hello({"sp": lax.rem(span + step, spans)})
    inner = jnp.where(chip > 0, 1, 0) + jnp.where(chip < chips - 1, 1, 0)
    pl.semaphore_wait(barrier, inner + spans)


def line_order(chips, visit):
    chip = tp_place()[0]
    for time in range(chips - 1):
        onward = chips - 1 - (time - chip)
        back = time - (chips - 1 - chip)
        pl.when((time >= chip) & (onward > chip))(lambda onward=onward: visit(onward, 0))
        pl.when((back >= 0) & (back < chip))(lambda back=back: visit(back, 1))
    visit(chip, None)


def column_loop(width, body):
    step = min(512, width)

    def one(index, carry):
        body(pl.ds(pl.multiple_of(index * step, step), step))
        return carry

    lax.fori_loop(0, width // step, one, 0)


def line_step(chips, block, way, term, width, total, travel, held, sent, landed):
    chip, _, _, before, after = tp_place()
    if way is None:

        def own(columns):
            total[:, columns] = term(columns)

        column_loop(width, own)
        return
    receives = chip > 0 if way == 0 else chip < chips - 1
    device = {"tp": after if way == 0 else before}
    copy = remote(
        travel.at[block], held.at[way, block], sent.at[block], landed.at[way, block], device
    )

    @pl.when(receives)
    def _():
        copy.wait_recv()

        def add(columns):
            travel[block, :, columns] = (
                term(columns) + held[way, block, :, columns].astype(jnp.float32)
            ).astype(jnp.bfloat16)

        column_loop(width, add)

    @pl.when(jnp.logical_not(receives))
    def _():
        def keep(columns):
            travel[block, :, columns] = term(columns).astype(jnp.bfloat16)

        column_loop(width, keep)

    copy.start()


def line_finish(chips, width, total, travel, held, sent, landed):
    chip, _, _, before, after = tp_place()
    for way, receives in ((0, chip > 0), (1, chip < chips - 1)):

        @pl.when(receives)
        def _(way=way):
            remote(
                travel.at[chip],
                held.at[way, chip],
                sent.at[chip],
                landed.at[way, chip],
                {"tp": after},
            ).wait_recv()

            def add(columns):
                total[:, columns] = total[:, columns] + held[way, chip, :, columns].astype(
                    jnp.float32
                )

            column_loop(width, add)

    for block in range(chips):
        copy = remote(
            travel.at[block], held.at[0, block], sent.at[block], landed.at[0, block], {"tp": after}
        )
        pl.when(chip != block)(copy.wait_send)


def sum_kernel(
    chips, parts, total, arrived, travel, held, core_sent, core_landed, sent, landed
):
    _, core, partner, _, _ = tp_place()
    width = parts.shape[-1]
    greet(chips, 1)

    def handed(block):
        return remote(
            parts.at[block, 1 - core],
            arrived.at[block],
            core_sent.at[block],
            core_landed.at[block],
            {"tp": partner},
        )

    line_order(chips, lambda block, way: handed(block).start())

    def visit(block, way):
        handed(block).wait_recv()

        def term(columns):
            return parts[block, core, :, columns].astype(jnp.float32) + arrived[
                block, :, columns
            ].astype(jnp.float32)

        line_step(chips, block, way, term, width, total, travel, held, sent, landed)

    line_order(chips, visit)
    line_finish(chips, width, total, travel, held, sent, landed)
    for block in range(chips):
        handed(block).wait_send()


def tp_sum(parts):
    chips, _, rows, width = parts.shape
    dma = pltpu.SemaphoreType.DMA
    return pl.pallas_call(
        functools.partial(sum_kernel, chips),
        out_shape=jax.ShapeDtypeStruct((rows, width), jnp.float32),
        in_specs=[VMEM],
        out_specs=VMEM,
        scratch_shapes=[
            pltpu.VMEM((chips, rows, width), jnp.bfloat16),
            pltpu.VMEM((chips, rows, width), jnp.bfloat16),
            pltpu.VMEM((2, chips, rows, width), jnp.bfloat16),
            dma((chips,)),
            dma((chips,)),
            dma((chips,)),
            dma((2, chips)),
        ],
        compiler_params=pltpu.CompilerParams(
            collective_id=0, has_side_effects=True, vmem_limit_bytes=min(60 << 20, 8 * parts.size + (6 << 20))
        ),
    )(parts)


def spread_kernel(
    chips,
    spans,
    picks,
    normed,
    notes,
    rows,
    all_notes,
    blocks,
    outgoing,
    line_sent,
    line_landed,
    note_sent,
    note_landed,
    span_sent,
    span_landed,
    core_sent,
    core_landed,
):
    chip, core, partner, before, after = tp_place()
    span = lax.axis_index("sp")
    count, width = normed.shape
    slots = rows.shape[3]
    greet(chips, spans)
    all_notes[chip] = notes[...]

    def pass_on(block, way, first):
        device = {"tp": after if way == 0 else before}
        return (
            remote(
                normed if first else blocks.at[block],
                blocks.at[block],
                line_sent.at[way, block],
                line_landed.at[block],
                device,
            ),
            remote(
                notes if first else all_notes.at[block],
                all_notes.at[block],
                note_sent.at[way, block],
                note_landed.at[block],
                device,
            ),
        )

    def to_span(block, step):
        other = lax.rem(span + step, spans)
        return remote(
            outgoing.at[block, other],
            rows.at[core, block, span],
            span_sent.at[block, step],
            span_landed.at[block, step],
            {"sp": other},
        )

    def to_partner(block):
        return remote(
            rows.at[core, block],
            rows.at[core, block],
            core_sent.at[block],
            core_landed.at[block],
            {"tp": partner},
        )

    def hand_out(block, source, note):
        listing = note[...][:picks, :count]
        slot = lax.broadcasted_iota(jnp.int32, (spans * slots, count), 0).astype(jnp.float32)
        chosen = jnp.zeros((spans * slots, count), jnp.float32)
        for pick in range(picks):
            chosen = jnp.where(slot == listing[pick : pick + 1], 1.0, chosen)
        chosen = chosen.astype(jnp.bfloat16)

        def select(columns):
            picked = jnp.dot(chosen, source[:, columns], preferred_element_type=jnp.float32)
            for expert in range(spans):
                outgoing[block, expert, :, columns] = picked[
                    expert * slots : (expert + 1) * slots
                ].astype(jnp.bfloat16)

        column_loop(width, select)
        for step in range(1, spans):
            to_span(block, step).start()
        rows[core, block, span] = outgoing[block, span]

    def start_both(block, way, first):
        for copy in pass_on(block, way, first):
            copy.start()

    pl.when(chip < chips - 1)(lambda: start_both(chip, 0, True))
    pl.when(chip > 0)(lambda: start_both(chip, 1, True))
    hand_out(chip, normed, notes)
    for step in range(1, chips):
        for way, block, present, further in (
            (0, chip - step, chip >= step, chip < chips - 1),
            (1, chip + step, chip + step < chips, chip > 0),
        ):

            @pl.when(present)
            def _(way=way, block=block, further=further):
                for copy in pass_on(block, way, False):
                    copy.wait_recv()
                pl.when(further)(lambda: start_both(block, way, False))
                hand_out(block, blocks.at[block], all_notes.at[block])

    def finish(block):
        for step in range(1, spans):
            to_span(block, step).wait_recv()
        to_partner(block).start()

    finish(chip)
    for step in range(1, chips):
        pl.when(chip >= step)(lambda step=step: finish(chip - step))
        pl.when(chip + step < chips)(lambda step=step: finish(chip + step))

    def wait_both(block, way, first):
        for copy in pass_on(block, way, first):
            copy.wait_send()

    for block in range(chips):
        pl.when((chip >= block) & (chip < chips - 1))(lambda block=block: wait_both(block, 0, False))
        pl.when((chip <= block) & (chip > 0))(lambda block=block: wait_both(block, 1, False))
        for step in range(1, spans):
            to_span(block, step).wait_send()
        to_partner(block).wait()


def spread(normed, notes, chips, spans, slots, picks):
    count, width = normed.shape
    dma = pltpu.SemaphoreType.DMA
    return pl.pallas_call(
        functools.partial(spread_kernel, chips, spans, picks),
        out_shape=(
            jax.ShapeDtypeStruct((2, chips, spans, slots, width), jnp.bfloat16),
            jax.ShapeDtypeStruct((chips,) + notes.shape, jnp.float32),
        ),
        in_specs=[VMEM, VMEM],
        out_specs=(VMEM, VMEM),
        scratch_shapes=[
            pltpu.VMEM((chips, count, width), jnp.bfloat16),
            pltpu.VMEM((chips, spans, slots, width), jnp.bfloat16),
            dma((2, chips)),
            dma((chips,)),
            dma((2, chips)),
            dma((chips,)),
            dma((chips, spans)),
            dma((chips, spans)),
            dma((chips,)),
            dma((chips,)),
        ],
        compiler_params=pltpu.CompilerParams(
            collective_id=1, has_side_effects=True, vmem_limit_bytes=min(60 << 20, 8 * chips * spans * slots * width + (8 << 20))
        ),
    )(normed, notes)


def collect_kernel(
    chips,
    spans,
    parts,
    shares,
    total,
    arrived,
    outgoing,
    gathered,
    travel,
    held,
    core_sent,
    core_landed,
    span_sent,
    span_landed,
    sent,
    landed,
):
    _, core, partner, _, _ = tp_place()
    span = lax.axis_index("sp")
    width = parts.shape[-1]
    greet(chips, spans)

    def handed(block):
        return remote(
            parts.at[1 - core, block],
            arrived.at[block],
            core_sent.at[block],
            core_landed.at[block],
            {"tp": partner},
        )

    def to_span(block, step):
        other = lax.rem(span + step, spans)
        return remote(
            outgoing.at[block, other],
            gathered.at[block, span],
            span_sent.at[block, step],
            span_landed.at[block, step],
            {"sp": other},
        )

    line_order(chips, lambda block, way: handed(block).start())

    def send_out(block, way):
        handed(block).wait_recv()

        def add(columns):
            outgoing[block, :, :, columns] = (
                parts[core, block, :, :, columns].astype(jnp.float32)
                + arrived[block, :, :, columns].astype(jnp.float32)
            ).astype(jnp.bfloat16)

        column_loop(width, add)
        for step in range(1, spans):
            to_span(block, step).start()
        gathered[block, span] = outgoing[block, span]

    line_order(chips, send_out)

    def visit(block, way):
        for step in range(1, spans):
            to_span(block, step).wait_recv()

        def term(columns):
            result = None
            for expert in range(spans):
                share = jnp.dot(
                    shares[block, expert],
                    gathered[block, expert, :, columns],
                    preferred_element_type=jnp.float32,
                )
                result = share if result is None else result + share
            return result

        line_step(chips, block, way, term, width, total, travel, held, sent, landed)

    line_order(chips, visit)
    line_finish(chips, width, total, travel, held, sent, landed)
    for block in range(chips):
        handed(block).wait_send()
        for step in range(1, spans):
            to_span(block, step).wait_send()


def collect(parts, shares):
    _, chips, spans, slots, width = parts.shape
    rows = shares.shape[2]
    dma = pltpu.SemaphoreType.DMA
    return pl.pallas_call(
        functools.partial(collect_kernel, chips, spans),
        out_shape=jax.ShapeDtypeStruct((rows, width), jnp.float32),
        in_specs=[VMEM, VMEM],
        out_specs=VMEM,
        scratch_shapes=[
            pltpu.VMEM((chips, spans, slots, width), jnp.bfloat16),
            pltpu.VMEM((chips, spans, slots, width), jnp.bfloat16),
            pltpu.VMEM((chips, spans, slots, width), jnp.bfloat16),
            pltpu.VMEM((chips, rows, width), jnp.bfloat16),
            pltpu.VMEM((2, chips, rows, width), jnp.bfloat16),
            dma((chips,)),
            dma((chips,)),
            dma((chips, spans)),
            dma((chips, spans)),
            dma((chips,)),
            dma((2, chips)),
        ],
        compiler_params=pltpu.CompilerParams(
            collective_id=2, has_side_effects=True, vmem_limit_bytes=min(60 << 20, 6 * parts.size + (8 << 20))
        ),
    )(parts, shares)


def local(
    queries,
    keys,
    values,
    doc_ids,
    sink_logits,
    out_weight,
    residual,
    norm_gain,
    routes,
    route_weights,
    gate_weight,
    up_weight,
    down_weight,
):
    span_rows = queries.shape[0]
    kv_width = keys.shape[1]
    kv_groups = kv_width // HEAD_DIM
    heads_here = queries.shape[1] // HEAD_DIM
    group_ratio = heads_here // kv_groups
    reach_back = WINDOW - 1
    score_scale = 1.0 / math.sqrt(HEAD_DIM)
    doc_float = (doc_ids + 1).astype(jnp.float32)
    tails = passed_along(
        jnp.concatenate(
            [
                keys[span_rows - reach_back :],
                values[span_rows - reach_back :],
                doc_float[span_rows - reach_back :, None].astype(jnp.bfloat16),
            ],
            axis=1,
        ),
        "sp",
        1,
    )
    all_keys = jnp.concatenate([tails[:, :kv_width], keys], axis=0)
    all_values = jnp.concatenate([tails[:, kv_width : 2 * kv_width], values], axis=0)
    all_docs = jnp.concatenate([tails[:, 2 * kv_width].astype(jnp.float32), doc_float], axis=0)
    block_rows = min(512, span_rows)
    sink_table = sink_logits.reshape(kv_groups, group_ratio, 1)
    offsets = (
        jnp.arange(block_rows)[:, None] + reach_back - jnp.arange(block_rows + reach_back)[None, :]
    )
    window_mask = (offsets >= 0) & (offsets <= reach_back)
    pieces = []
    for block_index in range(span_rows // block_rows):
        first_row = block_index * block_rows
        query_rows = queries[first_row : first_row + block_rows].reshape(
            block_rows, kv_groups, group_ratio, HEAD_DIM
        )
        key_rows = all_keys[first_row : first_row + block_rows + reach_back].reshape(
            block_rows + reach_back, kv_groups, HEAD_DIM
        )
        value_rows = all_values[first_row : first_row + block_rows + reach_back].reshape(
            block_rows + reach_back, kv_groups, HEAD_DIM
        )
        scores = (
            jnp.einsum("bgrd,sgd->grbs", query_rows, key_rows, preferred_element_type=jnp.float32)
            * score_scale
        )
        same_doc = (
            doc_float[first_row : first_row + block_rows][:, None]
            == all_docs[first_row : first_row + block_rows + reach_back][None, :]
        )
        scores = jnp.where(window_mask & same_doc, scores, masked_score)
        row_max = jnp.maximum(scores.max(-1), sink_table)
        exp_scores = jnp.exp(scores - row_max[..., None])
        denominator = exp_scores.sum(-1) + jnp.exp(sink_table - row_max)
        weighted = jnp.einsum(
            "grbs,sgd->bgrd",
            exp_scores.astype(jnp.bfloat16),
            value_rows,
            preferred_element_type=jnp.float32,
        )
        weighted = weighted / jnp.transpose(denominator, (2, 0, 1))[..., None]
        pieces.append(weighted.astype(jnp.bfloat16).reshape(block_rows, heads_here * HEAD_DIM))
    attended = jnp.concatenate(pieces, axis=0)
    rows_here = attended
    token_count, width = residual.shape
    chips = lax.axis_size("tp") // 2
    projected = tp_sum(
        jnp.dot(rows_here, out_weight, preferred_element_type=jnp.float32)
        .astype(jnp.bfloat16)
        .reshape(chips, 2, token_count, width)
    )
    stream = residual.astype(jnp.float32) + projected
    mean_value = stream.mean(-1, keepdims=True)
    centred = stream - mean_value
    variance = (centred * centred).mean(-1, keepdims=True)
    normed = (centred * lax.rsqrt(variance + layer_epsilon) * norm_gain).astype(jnp.bfloat16)
    spans = lax.axis_size("sp")
    route_count = routes.shape[1]
    capacity = 9 * route_count * token_count // (8 * spans)
    slots = -(-capacity // 8) * 8
    flat_routes = routes.reshape(-1)
    one_hot = (flat_routes[:, None] == jnp.arange(spans)[None, :]).astype(jnp.int32)
    slot_ids = jnp.sum((jnp.cumsum(one_hot, axis=0) - 1) * one_hot, axis=1)
    destination = (flat_routes * slots + slot_ids).astype(jnp.float32)
    notes = jnp.concatenate(
        [destination.reshape(token_count, route_count).T, route_weights.T], axis=0
    )
    notes = jnp.pad(
        notes,
        ((0, -2 * route_count % 8), (0, -token_count % 128)),
        constant_values=-1.0,
    )
    arrived, all_notes = spread(normed, notes, chips, spans, slots, route_count)
    rows_in = arrived.reshape(-1, width)
    gate = jnp.dot(rows_in, gate_weight[0], preferred_element_type=jnp.float32)
    upward = jnp.dot(rows_in, up_weight[0], preferred_element_type=jnp.float32)
    hidden = (jax.nn.silu(gate) * upward).astype(jnp.bfloat16)
    partial_value = jnp.dot(hidden, down_weight[0], preferred_element_type=jnp.float32).astype(
        jnp.bfloat16
    )
    places = all_notes[:, None, :route_count, :token_count, None]
    weights = all_notes[:, None, route_count : 2 * route_count, :token_count, None]
    slot_range = jnp.arange(spans * slots).astype(jnp.float32).reshape(1, spans, 1, 1, slots)
    shares = jnp.sum(jnp.where(places == slot_range, weights, 0.0), axis=2).astype(jnp.bfloat16)
    combined = collect(partial_value.reshape(arrived.shape), shares)
    return (stream + combined).astype(jnp.bfloat16)


def solution(mesh):
    placed = (
        P("sp", "tp"),
        P("sp", "tp"),
        P("sp", "tp"),
        P("sp"),
        P("tp"),
        P("tp", None),
        P(("sp", "tp"), None),
        P(),
        P(("sp", "tp"), None),
        P(("sp", "tp"), None),
        P("sp", None, "tp"),
        P("sp", None, "tp"),
        P("sp", "tp", None),
    )
    return jax.shard_map(
        local, mesh=mesh, in_specs=placed, out_specs=P(("sp", "tp"), None), check_vma=False
    )
```
